512 devices in a mesh: sp: 64 (over z, y), tp: 8 (over x, core).
Axes of the slice: x: 4, y: 4, z: 16, core: 2. Of those that a mesh axis runs over, the one named last changes fastest.
Arguments:
- tokens: bfloat16 [6144, 4, 1024], P(('sp', 'tp')), may hold values from -6 to 6
- in_gain: float32 [1024], replicated, may hold values from 0.1 to 1.9
- w_query: bfloat16 [1024, 1024], P('sp', 'tp'), may hold values from -0.1875 to 0.1875
- w_key: bfloat16 [1024, 1024], P('sp', 'tp'), may hold values from -0.1875 to 0.1875
- w_value: bfloat16 [1024, 1024], P('sp', 'tp'), may hold values from -0.1875 to 0.1875
- w_gate: bfloat16 [1024, 1024], P('sp', 'tp'), may hold values from -0.1875 to 0.1875
- w_beta: bfloat16 [1024, 8], P('sp', 'tp'), may hold values from -0.1875 to 0.1875
- conv_query: bfloat16 [4, 1024], P(None, 'tp'), may hold values from -3 to 3
- conv_key: bfloat16 [4, 1024], P(None, 'tp'), may hold values from -3 to 3
- conv_value: bfloat16 [4, 1024], P(None, 'tp'), may hold values from -3 to 3
- decay_rate: float32 [8], P('tp'), may hold values from 0.1 to 3
- out_gain: float32 [128], replicated, may hold values from 0.1 to 1.9
- w_out: bfloat16 [1024, 1024], P('tp', 'sp'), may hold values from -0.1875 to 0.1875
Outputs:
- mixed: bfloat16 [6144, 4, 1024], P(('sp', 'tp'))
The draws below stay inside these ranges and needn't reach their ends.
All inputs are finite; a program needn't handle non-finite values.
Results may differ from the reference program's by a relative error of at most 0.02.
Values may be sent and summed in bfloat16 or wider, within the bound.
A program may use at most 64 MiB of HBM per device.

```python
import math
import jax
import jax.numpy as jnp
from jax import lax

D = 1024
HEADS = 8
DK = 128
CONV_K = 4
BLOCK = 32
SEQS = 4
TOKENS = 6144


def shard_levels(own_key, extent, shards, low, top_value):
    level, own = 1.0, jax.random.fold_in(own_key, 6)
    for dim, parts in shards:
        heights = jnp.exp(jax.random.uniform(jax.random.fold_in(own, dim), (parts,), jnp.float32, low / len(shards), top_value / len(shards)))
        level = level * jnp.repeat(heights, extent[dim] // parts).reshape([-1 if axis == dim else 1 for axis in range(len(extent))])
    return level


def normal_values(stream_key, shape, spread, limit, shards=(), held_as=jnp.bfloat16):
    values = spread * jax.random.normal(stream_key, shape, jnp.float32)
    if shards:
        values = values * shard_levels(stream_key, shape, shards, -0.22, 0.18)
    return jnp.clip(values, -limit, limit).astype(held_as)


def setup_inputs(seed: int = 0) -> dict:
    key_of = jax.random.split(jax.random.key(seed), 14)
    tokens = normal_values(key_of[0], (TOKENS, SEQS, D), 1.0, 6.0, ((0, 512),))
    in_gain = jnp.clip(1.0 + 0.18 * jax.random.normal(key_of[1], (D,), jnp.float32), 0.1, 1.9)
    w_query = normal_values(key_of[2], (D, HEADS * DK), D ** -0.5, 0.1875, ((0, 64), (1, 8)))
    w_key = normal_values(key_of[3], (D, HEADS * DK), D ** -0.5, 0.1875, ((0, 64), (1, 8)))
    w_value = normal_values(key_of[4], (D, HEADS * DK), D ** -0.5, 0.1875, ((0, 64), (1, 8)))
    w_gate = normal_values(key_of[5], (D, HEADS * DK), D ** -0.5, 0.1875, ((0, 64), (1, 8)))
    w_beta = normal_values(key_of[6], (D, HEADS), D ** -0.5, 0.1875, ((0, 64), (1, 8)))
    conv_query = normal_values(key_of[7], (CONV_K, HEADS * DK), CONV_K ** -0.5, 3.0, ((1, 8),))
    conv_key = normal_values(key_of[8], (CONV_K, HEADS * DK), CONV_K ** -0.5, 3.0, ((1, 8),))
    conv_value = normal_values(key_of[9], (CONV_K, HEADS * DK), CONV_K ** -0.5, 3.0, ((1, 8),))
    decay_rate = jnp.clip(jnp.exp(math.log(3.0) - 3.4011974 * jax.random.uniform(key_of[10], (HEADS,), jnp.float32) ** shard_levels(key_of[10], (HEADS,), ((0, 8),), -0.2, 0.2)), 0.1, 3.0)
    out_gain = jnp.clip(1.0 + 0.18 * jax.random.normal(key_of[11], (DK,), jnp.float32), 0.1, 1.9)
    w_out = normal_values(key_of[12], (HEADS * DK, D), (HEADS * DK) ** -0.5, 0.1875, ((0, 8), (1, 64)))
    return {"tokens": tokens, "in_gain": in_gain, "w_query": w_query, "w_key": w_key, "w_value": w_value, "w_gate": w_gate, "w_beta": w_beta, "conv_query": conv_query, "conv_key": conv_key, "conv_value": conv_value, "decay_rate": decay_rate, "out_gain": out_gain, "w_out": w_out}


epsilon = 1e-06
out_epsilon = 1e-10
highest = lax.Precision.HIGHEST

def unit_inverse(lower):
    size = lower.shape[-1]
    inverse = jnp.eye(size, dtype=jnp.float32) - lower
    power = jnp.matmul(lower, lower, precision=highest)
    span = 2
    while span < size:
        inverse = inverse + jnp.matmul(inverse, power, precision=highest)
        power = jnp.matmul(power, power, precision=highest)
        span = span * 2
    return inverse

def make_terms(query, keys, values, beta, rate_col):
    size = query.shape[-2]
    steps = jnp.arange(1, size + 1).astype(jnp.float32)
    cumulative = -rate_col * steps
    lower_mask = jnp.tril(jnp.ones((size, size), bool))
    strict_mask = jnp.tril(jnp.ones((size, size), bool), -1)
    decay = jnp.where(lower_mask, jnp.exp(cumulative[..., :, None] - cumulative[..., None, :]), 0.0)
    weighted = keys * beta[..., None]
    lower = jnp.where(strict_mask, jnp.einsum('...cd,...sd->...cs', weighted, keys, precision=highest) * decay, 0.0)
    inverse = unit_inverse(lower)
    update = jnp.einsum('...cs,...sv->...cv', inverse, values * beta[..., None], precision=highest)
    erase = jnp.einsum('...cs,...sd->...cd', inverse, weighted * jnp.exp(cumulative)[..., None], precision=highest)
    scores = jnp.einsum('...cd,...sd->...cs', query, keys, precision=highest) * decay
    query_decayed = query * jnp.exp(cumulative)[..., None]
    final = cumulative[..., -1:]
    keys_decayed = keys * jnp.exp(final - cumulative)[..., None]
    return (query_decayed, keys_decayed, update, erase, scores, jnp.exp(final))

def apply_block(state, terms):
    query_decayed, keys_decayed, update, erase, scores, kept = terms
    fresh = update - jnp.einsum('...cd,...dv->...cv', erase, state, precision=highest)
    output = jnp.einsum('...cd,...dv->...cv', query_decayed, state, precision=highest)
    output = output + jnp.einsum('...cs,...sv->...cv', scores, fresh, precision=highest)
    state = state * kept[..., None] + jnp.einsum('...cd,...cv->...dv', keys_decayed, fresh, precision=highest)
    return (state, output)

def causal_conv(pre, conv_taps, history):
    width = conv_taps.shape[0]
    extended = jnp.concatenate([history, pre], axis=0).astype(jnp.float32)
    length = pre.shape[0]
    total = jnp.zeros(pre.shape, jnp.float32)
    for tap in range(width):
        total = total + extended[tap:tap + length] * conv_taps[tap].astype(jnp.float32)
    return total

def rms_scale(values_in, gain):
    values = values_in.astype(jnp.float32)
    scaled = values * lax.rsqrt(lax.optimization_barrier(jnp.mean(values * values, axis=-1, keepdims=True)) + epsilon)
    return (scaled * gain).astype(jnp.bfloat16)

def l2_normalize(array):
    return array * lax.rsqrt(lax.optimization_barrier(jnp.sum(array * array, axis=-1, keepdims=True)) + epsilon)

def finish(outputs, out_gain, gate_pre):
    normed = outputs * lax.rsqrt(lax.optimization_barrier(jnp.mean(outputs * outputs, axis=-1, keepdims=True)) + out_epsilon) * out_gain
    gate = jax.nn.silu(gate_pre.astype(jnp.float32)).reshape(outputs.shape)
    return (normed * gate).astype(jnp.bfloat16).reshape(outputs.shape[0], outputs.shape[1], -1)

def reference(tokens, in_gain, w_query, w_key, w_value, w_gate, w_beta, conv_query, conv_key, conv_value, decay_rate, out_gain, w_out):
    width = tokens.shape[2]
    head_width = HEADS * DK
    normed = rms_scale(tokens, in_gain)
    flat = normed.reshape(-1, width)

    def project(weight):
        return jnp.dot(flat, weight, preferred_element_type=jnp.float32).astype(jnp.bfloat16).reshape(TOKENS, SEQS, -1)
    mixed_pre = jnp.concatenate([project(w_query), project(w_key), project(w_value)], axis=2)
    gate_pre = project(w_gate)
    beta_pre = project(w_beta)
    history = jnp.zeros((CONV_K - 1, SEQS, 3 * head_width), jnp.bfloat16)
    conv_taps = jnp.concatenate([conv_query, conv_key, conv_value], axis=1)
    convolved = jax.nn.silu(causal_conv(mixed_pre, conv_taps, history))

    def split_heads(array):
        return array.reshape(TOKENS, SEQS, HEADS, DK)
    query = l2_normalize(split_heads(convolved[:, :, :head_width])) * DK ** (-0.5)
    keys = l2_normalize(split_heads(convolved[:, :, head_width:2 * head_width]))
    values = split_heads(convolved[:, :, 2 * head_width:])
    beta = jax.nn.sigmoid(beta_pre.astype(jnp.float32) + math.log(DK / (4.0 * TOKENS)))
    rate_col = (decay_rate / TOKENS)[:, None]
    blocks = TOKENS // BLOCK

    def to_blocks(array):
        return jnp.moveaxis(array.reshape(blocks, BLOCK, SEQS, HEADS, DK), 1, 3)
    beta_blocks = jnp.moveaxis(beta.reshape(blocks, BLOCK, SEQS, HEADS), 1, 3)

    def advance(state, inputs):
        query_block, key_block, value_block, beta_block = inputs
        return apply_block(state, make_terms(query_block, key_block, value_block, beta_block, rate_col))
    initial = jnp.zeros((SEQS, HEADS, DK, DK), jnp.float32)
    _, outputs = lax.scan(advance, initial, (to_blocks(query), to_blocks(keys), to_blocks(values), beta_blocks))
    outputs = jnp.moveaxis(outputs, 3, 1).reshape(TOKENS, SEQS, HEADS, DK)
    gated = finish(outputs, out_gain, gate_pre)
    mixed = jnp.dot(gated.reshape(-1, head_width), w_out, preferred_element_type=jnp.float32).astype(jnp.bfloat16)
    return mixed.reshape(TOKENS, SEQS, width)
```

```python
import functools
import math

import jax
import jax.numpy as jnp
from jax import lax
from jax.experimental import pallas as pl
from jax.experimental.pallas import tpu as pltpu
from jax.sharding import Mesh
from jax.sharding import PartitionSpec as P

MESH = pl.DeviceIdType.MESH
DK = 128
TAPS = 4
INNER = 32
ROWS = 16
f32, bf16 = jnp.float32, jnp.bfloat16
epsilon = 1e-06
out_epsilon = 1e-10
SP = ("z", "y")
TP = ("x", "c")


def copy_to(src, dst, send, recv, device):
    return pltpu.make_async_remote_copy(
        src_ref=src, dst_ref=dst, send_sem=send, recv_sem=recv, device_id=device, device_id_type=MESH
    )


def dot(a, b):
    return jnp.dot(a.astype(bf16), b.astype(bf16), preferred_element_type=f32)


def dot_nt(a, b):
    return lax.dot_general(
        a.astype(bf16), b.astype(bf16), (((1,), (1,)), ((), ())), preferred_element_type=f32
    )


def mixer(
    dims, x_ref, w_ref, b_ref, taps_ref, rate_ref, gain_ref, out_ref,
    wbuf, bbuf, wbt, xbuf, hin, ext, bext, qs, ks, vs, bs, olo, rdo, mbuf, wo, gsend, grecv, obuf,
    wy_s, wy_r, by_s, by_r, wz_s, wz_r, bz_s, bz_r, xy_s, xy_r, hz_s, hz_r, hy_s, hy_r, hx_s, hx_r,
    hc_s, hc_r, xx_s, xx_r, xc_s, xc_r, ox_s, ox_r, oc_s, oc_r, mz_s, mz_r, g_s, g_r, o_s, o_r, l_s,
):
    Z, Y, X, NB, PB, CH = dims
    TPN = 2 * X
    NT = Y * TPN * NB
    D = wo.shape[2]
    z, y, x, c = (lax.axis_index(a) for a in ("z", "y", "x", "c"))
    tp = x * 2 + c
    NP, NM = Z // 2, (Z - 1) // 2
    up = (lax.rem(z + 1, Z), y, x, c)
    down = (lax.rem(z + Z - 1, Z), y, x, c)
    sib = (z, y, x, 1 - c)

    def ymod(k):
        return lax.rem(y + k, Y)

    def xmod(k):
        return lax.rem(x + k, X)

    def zmod(k):
        return lax.rem(z + k + Z, Z)

    barrier = pltpu.get_barrier_semaphore()
    peers = [up, down] + [(z, ymod(k), x, c) for k in range(1, Y)]
    peers += [(z, y, lax.rem(tp + k, TPN) // 2, lax.rem(lax.rem(tp + k, TPN), 2)) for k in range(1, TPN)]
    for peer in peers:
        pl.semaphore_signal(barrier, inc=1, device_id=peer, device_id_type=MESH)
    pl.semaphore_wait(barrier, len(peers))

    copies = []

    def go(cp):
        cp.start()
        copies.append(cp)

    def rows_of(zz, yy):
        return pl.ds(pl.multiple_of((zz * Y + yy) * ROWS, ROWS), ROWS)

    own = rows_of(z, y)
    local = pltpu.make_async_copy(w_ref, wbuf.at[own], l_s.at[0])
    local.start()
    local_b = pltpu.make_async_copy(b_ref, bbuf.at[z, y], l_s.at[1])
    local_b.start()
    for k in range(1, Y):
        go(copy_to(w_ref, wbuf.at[own], wy_s.at[k], wy_r.at[k], (z, ymod(k), x, c)))
        go(copy_to(b_ref, bbuf.at[z, y], by_s.at[k], by_r.at[k], (z, ymod(k), x, c)))
    go(copy_to(w_ref, wbuf.at[own], wz_s.at[0, 1, 0], wz_r.at[0, 1, 0], up))
    if NM:
        go(copy_to(w_ref, wbuf.at[own], wz_s.at[1, 1, 0], wz_r.at[1, 1, 0], down))
    slot0 = tp * Y
    for k in range(1, Y):
        go(copy_to(x_ref.at[ymod(k)], xbuf.at[slot0 + y], xy_s.at[k], xy_r.at[k], (z, ymod(k), x, c)))
    local_x = pltpu.make_async_copy(x_ref.at[y], xbuf.at[slot0 + y], l_s.at[2])
    local_x.start()
    HALO = TPN * Y
    last_tp = jnp.logical_and(x == X - 1, c == 1)
    tail_owner = jnp.logical_and(last_tp, y == Y - 1)

    @pl.when(tail_owner)
    def _():
        copy_to(x_ref, hin, hz_s, hz_r, up).start()

    for k in range(1, Y):
        blk = rows_of(z, ymod(Y - k))
        copy_to(w_ref, wbuf.at[blk], wy_s.at[k], wy_r.at[k], sib).wait_recv()
    for d in range(1, Y):
        blk = rows_of(z, ymod(d))
        go(copy_to(wbuf.at[blk], wbuf.at[blk], wz_s.at[0, 1, d], wz_r.at[0, 1, d], up))
        if NM:
            go(copy_to(wbuf.at[blk], wbuf.at[blk], wz_s.at[1, 1, d], wz_r.at[1, 1, d], down))
    for k in range(1, Y):
        copy_to(b_ref, bbuf.at[z, ymod(Y - k)], by_s.at[k], by_r.at[k], sib).wait_recv()
    local_b.wait()
    go(copy_to(bbuf.at[z], bbuf.at[z], bz_s.at[0, 1], bz_r.at[0, 1], up))
    if NM:
        go(copy_to(bbuf.at[z], bbuf.at[z], bz_s.at[1, 1], bz_r.at[1, 1], down))

    for k in range(1, Y):
        copy_to(x_ref.at[0], xbuf.at[slot0 + ymod(Y - k)], xy_s.at[k], xy_r.at[k], sib).wait_recv()
    local_x.wait()
    mine = pl.ds(slot0, Y)
    for k in range(1, X):
        go(copy_to(xbuf.at[mine], xbuf.at[mine], xx_s.at[k], xx_r.at[k], (z, y, xmod(k), c)))
    go(copy_to(xbuf.at[mine], xbuf.at[mine], xc_s.at[0], xc_r.at[0], sib))

    def w_step(k, plus, fplus, minus, fminus):
        for d in range(Y):
            if plus:
                blk = rows_of(zmod(-k), ymod(d))
                copy_to(wbuf.at[blk], wbuf.at[blk], wz_s.at[0, k, d], wz_r.at[0, k, d], up).wait_recv()
                if fplus:
                    copy_to(wbuf.at[blk], wbuf.at[blk], wz_s.at[0, k + 1, d], wz_r.at[0, k + 1, d], up).start()
            if minus:
                blk = rows_of(zmod(k), ymod(d))
                copy_to(wbuf.at[blk], wbuf.at[blk], wz_s.at[1, k, d], wz_r.at[1, k, d], down).wait_recv()
                if fminus:
                    copy_to(wbuf.at[blk], wbuf.at[blk], wz_s.at[1, k + 1, d], wz_r.at[1, k + 1, d], down).start()
        if plus:
            g = bbuf.at[zmod(-k)]
            copy_to(g, g, bz_s.at[0, k], bz_r.at[0, k], up).wait_recv()
            if fplus:
                copy_to(g, g, bz_s.at[0, k + 1], bz_r.at[0, k + 1], up).start()
        if minus:
            g = bbuf.at[zmod(k)]
            copy_to(g, g, bz_s.at[1, k], bz_r.at[1, k], down).wait_recv()
            if fminus:
                copy_to(g, g, bz_s.at[1, k + 1], bz_r.at[1, k + 1], down).start()

    def ring(step):
        both = max(min(NP - 1, NM - 1), 0)
        if both:

            @pl.loop(1, both + 1)
            def _(k):
                step(k, True, True, True, True)

        for k in range(both + 1, NP + 1):
            step(k, True, k < NP, k <= NM, k < NM)

    def token_forwards():
        @pl.when(tail_owner)
        def _():
            copy_to(x_ref, hin, hz_s, hz_r, up).wait_recv()
            for k in range(1, Y):
                copy_to(hin.at[ymod(k)], xbuf.at[HALO], hy_s.at[k], hy_r, (z, ymod(k), x, c)).start()
            cp = pltpu.make_async_copy(hin.at[y], xbuf.at[HALO], l_s.at[3])
            cp.start()
            cp.wait()

        @pl.when(jnp.logical_and(last_tp, y != Y - 1))
        def _():
            copy_to(hin.at[0], xbuf.at[HALO], hy_s.at[0], hy_r, sib).wait_recv()

        @pl.when(last_tp)
        def _():
            for k in range(1, X):
                copy_to(xbuf.at[HALO], xbuf.at[HALO], hx_s.at[k], hx_r, (z, y, xmod(k), c)).start()

        for k in range(1, X):
            got = pl.ds((xmod(X - k) * 2 + c) * Y, Y)
            copy_to(xbuf.at[got], xbuf.at[got], xx_s.at[k], xx_r.at[k], sib).wait_recv()
            go(copy_to(xbuf.at[got], xbuf.at[got], xc_s.at[k], xc_r.at[k], sib))

        @pl.when(c == 1)
        def _():
            @pl.when(x != X - 1)
            def _():
                copy_to(xbuf.at[HALO], xbuf.at[HALO], hx_s.at[0], hx_r, sib).wait_recv()

            copy_to(xbuf.at[HALO], xbuf.at[HALO], hc_s, hc_r, sib).start()

    w_step_early = min(2, NP - 1)
    token_forwards()
    ring(w_step)

    sc = (1 - c)
    for k in range(X):
        got = pl.ds((xmod(X - k) * 2 + sc) * Y, Y)
        copy_to(xbuf.at[got], xbuf.at[got], xc_s.at[k], xc_r.at[k], sib).wait_recv()

    @pl.when(c == 0)
    def _():
        copy_to(xbuf.at[HALO], xbuf.at[HALO], hc_s, hc_r, sib).wait_recv()

    local.wait()

    PR = TPN * Y * PB
    xs = xbuf[...].reshape(PR + PB, D)
    pre = jnp.dot(xs, wbuf[:, : 4 * DK], preferred_element_type=f32).astype(bf16).astype(f32)
    bsum = jnp.sum(bbuf[...].reshape(D // DK, 8, DK), axis=1)
    for j in range(D // DK):
        wbt[:, j * DK : (j + 1) * DK] = jnp.broadcast_to(bsum[j : j + 1, :], (DK, DK)).astype(bf16)
    bpre = dot_nt(xs, wbt[...]).astype(bf16).astype(f32)
    started = jnp.where(z > 0, 1.0, 0.0).astype(f32)
    ext[8 - (TAPS - 1) : 8, :] = pre[PR + NB - (TAPS - 1) : PR + NB, :] * started
    for yy in range(Y):
        for t in range(TPN):
            row = (t * Y + yy) * PB
            to = (yy * TPN + t) * NB
            ext[8 + to : 8 + to + NB, :] = pre[row : row + NB, :]
            bext[to : to + NB, :] = bpre[row : row + NB, :]

    for j in range(D // DK):
        tile = wbuf[j * DK : (j + 1) * DK, 4 * DK : 5 * DK].astype(f32)
        wo[tp, :, j * DK : (j + 1) * DK] = tile.T.astype(bf16)

    outs = []
    for kind in range(3):
        lanes = slice(kind * DK, (kind + 1) * DK)
        acc = jnp.zeros((NT, DK), f32)
        for j in range(TAPS):
            at = 8 - (TAPS - 1) + j
            acc = acc + ext[at : at + NT, lanes] * taps_ref[j : j + 1, lanes]
        outs.append(acc * jax.nn.sigmoid(acc))
    q, k_, v = outs
    qs[...] = q * (lax.rsqrt(jnp.sum(q * q, axis=1, keepdims=True) + epsilon) * DK ** (-0.5))
    ks[...] = k_ * lax.rsqrt(jnp.sum(k_ * k_, axis=1, keepdims=True) + epsilon)
    vs[...] = v
    total_tokens = NT * Z
    bs[...] = jax.nn.sigmoid(bext[...] + math.log(DK / (4.0 * total_tokens)))

    for k in range(1, X):
        go(copy_to(wo.at[tp], wo.at[tp], ox_s.at[k], ox_r.at[k], (z, y, xmod(k), c)))
    go(copy_to(wo.at[tp], wo.at[tp], oc_s.at[0], oc_r.at[0], sib))

    rate = rate_ref[...]
    ri = lax.broadcasted_iota(jnp.int32, (CH, CH), 0)
    ci = lax.broadcasted_iota(jnp.int32, (CH, CH), 1)
    rl = lax.broadcasted_iota(jnp.int32, (CH, DK), 0).astype(f32)
    rate_c = rate_ref[:, :CH]
    decay = jnp.where(ri >= ci, jnp.exp(-rate_c * (ri - ci).astype(f32)), 0.0)
    down_row = jnp.exp(-rate * (rl + 1.0))
    up_row = jnp.exp(-rate * (CH - 1.0 - rl))
    kept = jnp.exp(-rate * CH)
    eye = jnp.where(
        lax.broadcasted_iota(jnp.int32, (DK, DK), 0) == lax.broadcasted_iota(jnp.int32, (DK, DK), 1), 1.0, 0.0
    ).astype(f32)
    prefix = None
    for i in range(NT // CH):
        rows = slice(i * CH, (i + 1) * CH)
        q, k_, v, b = qs[rows, :], ks[rows, :], vs[rows, :], bs[rows, :]
        kb = k_ * b
        lower = jnp.where(ri > ci, dot_nt(kb, k_) * decay, 0.0)
        scores = dot_nt(q, k_) * decay
        near = jnp.where(ri // INNER == ci // INNER, lower, 0.0)
        inverse = jnp.where(ri == ci, 1.0, 0.0) - near
        power = dot(near, near)
        span = 2
        while span < INNER:
            inverse = inverse + dot(inverse, power)
            span *= 2
            if span < INNER:
                power = dot(power, power)
        span = INNER
        while span < CH:
            part = jnp.where(
                jnp.logical_and(ri // (2 * span) == ci // (2 * span), ri // span != ci // span), lower, 0.0
            )
            inverse = inverse - dot(inverse, dot(part, inverse))
            span *= 2
        both = dot(inverse, jnp.concatenate([kb * down_row, v * b], axis=1))
        inner = dot(scores, both)
        reach = q * down_row - inner[:, :DK]
        kd = (k_ * up_row).T
        tail = dot(kd, both)
        step_map = kept * eye - tail[:, :DK]
        if prefix is None:
            rdo[rows, :] = reach
            olo[rows, :] = inner[:, DK:]
            prefix = jnp.concatenate([step_map, tail[:, DK:]], axis=1)
        else:
            seen = dot(reach, prefix)
            rdo[rows, :] = seen[:, :DK]
            olo[rows, :] = inner[:, DK:] + seen[:, DK:]
            prefix = dot(step_map, prefix)
            prefix = jnp.concatenate([prefix[:, :DK], prefix[:, DK:] + tail[:, DK:]], axis=1)
    kappa = jnp.exp(-rate * NT)
    mbuf[z, :, :DK] = (prefix[:, :DK] - kappa * eye).astype(bf16)
    mbuf[z, :, DK:] = prefix[:, DK:].astype(bf16)

    NCH = mz_s.shape[2]
    PIECE = DK // NCH

    def piece(zz, d):
        return mbuf.at[zz, pl.ds(d * PIECE, PIECE)]

    for d in range(NCH):
        go(copy_to(piece(z, d), piece(z, d), mz_s.at[0, 1, d], mz_r.at[0, 1, d], up))
        if NM:
            go(copy_to(piece(z, d), piece(z, d), mz_s.at[1, 1, d], mz_r.at[1, 1, d], down))

    near_d, near_u, far = ext.at[0:DK, 0:DK], ext.at[0:DK, DK : 2 * DK], ext.at[0:DK, 2 * DK : 3 * DK]

    near_d[...] = jnp.zeros((DK, DK), f32)
    near_u[...] = jnp.zeros((DK, DK), f32)
    far[...] = jnp.zeros((DK, DK), f32)

    def m_step(k, plus, fplus, minus, fminus):
        for d in range(NCH):
            if plus:
                p = piece(zmod(-k), d)
                copy_to(p, p, mz_s.at[0, k, d], mz_r.at[0, k, d], up).wait_recv()
                if fplus:
                    copy_to(p, p, mz_s.at[0, k + 1, d], mz_r.at[0, k + 1, d], up).start()
            if minus:
                p = piece(zmod(k), d)
                copy_to(p, p, mz_s.at[1, k, d], mz_r.at[1, k, d], down).wait_recv()
                if fminus:
                    copy_to(p, p, mz_s.at[1, k + 1, d], mz_r.at[1, k + 1, d], down).start()
        if plus:
            got = mbuf[zmod(-k)]
            kk = k * 1.0 if isinstance(k, int) else k.astype(f32)
            scale = jnp.exp(-rate * NT * (kk - 1.0))
            valid = jnp.where(z >= k, 1.0, 0.0).astype(f32)
            nd, nu = near_d[...], near_u[...]
            prod = dot(nd, got)
            gd, gu = got[:, :DK].astype(f32), got[:, DK:].astype(f32)
            near_d[...] = kappa * nd + scale * gd + prod[:, :DK]
            near_u[...] = nu + valid * (scale * gu + prod[:, DK:])
        if minus:
            got = mbuf[zmod(k)]
            valid = jnp.where(z + k >= Z, 1.0, 0.0).astype(f32)
            s = far[...]
            far[...] = kappa * s + dot(got[:, :DK], s) + valid * got[:, DK:].astype(f32)

    ring(m_step)

    for k in range(1, X):
        h = xmod(X - k) * 2 + c
        copy_to(wo.at[h], wo.at[h], ox_s.at[k], ox_r.at[k], sib).wait_recv()
        go(copy_to(wo.at[h], wo.at[h], oc_s.at[k], oc_r.at[k], sib))

    s = far[...]
    state = jnp.exp(-rate * NT * NP) * s + dot(near_d[...], s) + near_u[...]
    o = olo[...] + dot(rdo[...], state)
    gate = ext[8 : 8 + NT, 3 * DK : 4 * DK]
    o = o * lax.rsqrt(jnp.mean(o * o, axis=1, keepdims=True) + out_epsilon) * gain_ref[...]
    olo[...] = o * (gate * jax.nn.sigmoid(gate))
    for yy in range(Y):
        for t in range(TPN):
            to = (yy * TPN + t) * NB
            gsend[t, yy, 0:NB, :] = olo[to : to + NB, :].astype(bf16)
    for k in range(1, TPN):
        t = lax.rem(tp + k, TPN)
        go(copy_to(gsend.at[t], grecv.at[tp], g_s.at[k], g_r.at[k], (z, y, t // 2, lax.rem(t, 2))))
    grecv[tp] = gsend[tp]
    for k in range(X):
        h = xmod(X - k) * 2 + sc
        copy_to(wo.at[h], wo.at[h], oc_s.at[k], oc_r.at[k], sib).wait_recv()
    for k in range(1, TPN):
        t = lax.rem(tp + TPN - k, TPN)
        copy_to(gsend.at[0], grecv.at[t], g_s.at[k], g_r.at[k], sib).wait_recv()
    gated = jnp.concatenate([grecv[t].reshape(Y * PB, DK) for t in range(TPN)], axis=1)
    res = jnp.dot(gated, wo[...].reshape(TPN * DK, D), preferred_element_type=f32)
    obuf[0] = res.astype(bf16).reshape(Y, PB, D)
    for k in range(1, Y):
        go(copy_to(obuf.at[0, ymod(k)], obuf.at[1, y], o_s.at[k], o_r.at[k], (z, ymod(k), x, c)))
    out_ref[y] = obuf[0, y]
    for k in range(1, Y):
        src = ymod(Y - k)
        copy_to(obuf.at[0, 0], obuf.at[1, src], o_s.at[k], o_r.at[k], sib).wait_recv()
        out_ref[src] = obuf[1, src]

    for cp in copies:
        cp.wait_send()
    for d, steps in ((0, NP), (1, NM)):
        for k in range(2, steps + 1):
            to = up if d == 0 else down
            for e in range(Y):
                copy_to(w_ref, wbuf.at[own], wz_s.at[d, k, e], wz_r.at[d, k, e], to).wait_send()
            copy_to(bbuf.at[0], bbuf.at[0], bz_s.at[d, k], bz_r.at[d, k], to).wait_send()
            for e in range(NCH):
                copy_to(piece(z, e), piece(z, e), mz_s.at[d, k, e], mz_r.at[d, k, e], to).wait_send()

    @pl.when(tail_owner)
    def _():
        copy_to(x_ref, hin, hz_s, hz_r, up).wait_send()
        for k in range(1, Y):
            copy_to(hin.at[0], xbuf.at[HALO], hy_s.at[k], hy_r, sib).wait_send()

    @pl.when(last_tp)
    def _():
        for k in range(1, X):
            copy_to(xbuf.at[HALO], xbuf.at[HALO], hx_s.at[k], hx_r, sib).wait_send()

    @pl.when(c == 1)
    def _():
        copy_to(xbuf.at[HALO], xbuf.at[HALO], hc_s, hc_r, sib).wait_send()


def shards(
    sizes, tokens, in_gain, w_query, w_key, w_value, w_gate, w_beta,
    conv_query, conv_key, conv_value, decay_rate, out_gain, w_out,
):
    Z, Y, X = sizes
    NB, seqs, D = tokens.shape
    PB = -(-NB // 16) * 16
    TPN = 2 * X
    NT = Y * TPN * NB
    CH = 128 if NT % 128 == 0 else 96
    NCH = 4
    values = tokens.astype(f32)
    scaled = values * lax.rsqrt(jnp.mean(values * values, axis=-1, keepdims=True) + epsilon)
    normed = jnp.swapaxes((scaled * in_gain).astype(bf16), 0, 1)
    normed = jnp.pad(normed, ((0, 0), (0, PB - NB), (0, 0)))
    w = jnp.concatenate([w_query, w_key, w_value, w_gate, w_out.T], axis=1)
    part = lax.rem(lax.axis_index(SP), 8)
    lane = lax.broadcasted_iota(jnp.int32, (1, DK), 1)
    b = jnp.where(lane // ROWS == part, jnp.tile(w_beta.astype(f32).reshape(1, ROWS), (1, 8)), 0.0)
    taps = jnp.concatenate([conv_query, conv_key, conv_value], axis=1).astype(f32)
    rate = jnp.broadcast_to((decay_rate / (NT * Z)).reshape(1, 1), (1, DK))
    D1 = pltpu.SemaphoreType.DMA
    NP = Z // 2
    scratch = [
        pltpu.VMEM((D, 5 * DK), bf16),
        pltpu.VMEM((Z, Y, 1, DK), f32),
        pltpu.VMEM((DK, D), bf16),
        pltpu.VMEM((TPN * Y + 1, PB, D), bf16),
        pltpu.VMEM((Y, PB, D), bf16),
        pltpu.VMEM((8 + max(NT, DK), 4 * DK), f32),
        pltpu.VMEM((NT, DK), f32),
        pltpu.VMEM((NT, DK), f32),
        pltpu.VMEM((NT, DK), f32),
        pltpu.VMEM((NT, DK), f32),
        pltpu.VMEM((NT, DK), f32),
        pltpu.VMEM((NT, DK), f32),
        pltpu.VMEM((NT, DK), f32),
        pltpu.VMEM((Z, DK, 2 * DK), bf16),
        pltpu.VMEM((TPN, DK, D), bf16),
        pltpu.VMEM((TPN, Y, PB, DK), bf16),
        pltpu.VMEM((TPN, Y, PB, DK), bf16),
        pltpu.VMEM((2, Y, PB, D), bf16),
    ]
    sems = [
        D1((Y,)), D1((Y,)), D1((Y,)), D1((Y,)),
        D1((2, NP + 1, Y)), D1((2, NP + 1, Y)), D1((2, NP + 1)), D1((2, NP + 1)),
        D1((Y,)), D1((Y,)), D1(()), D1(()), D1((Y,)), D1(()), D1((X,)), D1(()),
        D1(()), D1(()), D1((X,)), D1((X,)), D1((X,)), D1((X,)),
        D1((X,)), D1((X,)), D1((X,)), D1((X,)),
        D1((2, NP + 1, NCH)), D1((2, NP + 1, NCH)), D1((TPN,)), D1((TPN,)), D1((Y,)), D1((Y,)), D1((4,)),
    ]
    vmem = pl.BlockSpec(memory_space=pltpu.VMEM)
    out = pl.pallas_call(
        functools.partial(mixer, (Z, Y, X, NB, PB, CH)),
        out_shape=jax.ShapeDtypeStruct((Y, PB, D), bf16),
        in_specs=[vmem] * 6,
        out_specs=vmem,
        scratch_shapes=scratch + sems,
        compiler_params=pltpu.CompilerParams(collective_id=0, has_side_effects=True, vmem_limit_bytes=48 * 2**20),
        name="mixer",
    )(normed, w, b, taps, rate, out_gain.reshape(1, DK))
    return jnp.swapaxes(out[:, :NB], 0, 1)


def solution(mesh, sizes=(16, 4, 4)):
    Z, Y, X = sizes
    finer = Mesh(mesh.devices.reshape(Z, Y, X, 2), ("z", "y", "x", "c"))
    return jax.shard_map(
        functools.partial(shards, sizes),
        mesh=finer,
        in_specs=(
            P(SP + TP, None, None), P(), P(SP, TP), P(SP, TP), P(SP, TP), P(SP, TP), P(SP, TP),
            P(None, TP), P(None, TP), P(None, TP), P(TP), P(), P(TP, SP),
        ),
        out_specs=P(SP + TP, None, None),
        check_vma=False,
    )
```

```python
import functools
import math

import jax
import jax.numpy as jnp
from jax import lax
from jax.experimental import pallas as pl
from jax.experimental.pallas import tpu as pltpu
from jax.sharding import Mesh
from jax.sharding import PartitionSpec as P

MESH = pl.DeviceIdType.MESH
DK = 128
TAPS = 4
INNER = 32
ROWS = 16
f32, bf16 = jnp.float32, jnp.bfloat16
epsilon = 1e-06
out_epsilon = 1e-10
SP = ("z", "y")
TP = ("x", "c")


def copy_to(src, dst, send, recv, device):
    return pltpu.make_async_remote_copy(
        src_ref=src, dst_ref=dst, send_sem=send, recv_sem=recv, device_id=device, device_id_type=MESH
    )


PHASES = False
open_scopes = []


def phase(name):
    if PHASES:
        while open_scopes:
            open_scopes.pop().__exit__(None, None, None)
        if name:
            open_scopes.append(jax.named_scope(name))
            open_scopes[-1].__enter__()


def dot(a, b):
    return jnp.dot(a.astype(bf16), b.astype(bf16), preferred_element_type=f32)


def dot_nt(a, b):
    return lax.dot_general(
        a.astype(bf16), b.astype(bf16), (((1,), (1,)), ((), ())), preferred_element_type=f32
    )


def mixer(
    dims, tok_hbm, ing_hbm, wq_hbm, wk_hbm, wv_hbm, wg_hbm, wo_hbm, wb_hbm, cq_hbm, ck_hbm, cv_hbm, dr_hbm,
    og_hbm, out_ref, tok, tokf, ing, x_ref, w_ref, b16, b_ref, taps_b, dr, gain_ref, in_s,
    wbuf, bbuf, wbt, xbuf, hin, ext, bext, qs, ks, vs, bs, olo, rdo, mbuf, wo, gsend, grecv, obuf,
    wy_s, wy_r, by_s, by_r, wz_s, wz_r, bz_s, bz_r, xy_s, xy_r, hz_s, hz_r, hy_s, hy_r, hx_s, hx_r,
    hc_s, hc_r, xx_s, xx_r, xc_s, xc_r, ox_s, ox_r, oc_s, oc_r, mz_s, mz_r, g_s, g_r, o_s, o_r, l_s,
):
    Z, Y, X, NB, PB, CH = dims
    TPN = 2 * X
    NT = Y * TPN * NB
    D = wo.shape[2]
    z, y, x, c = (lax.axis_index(a) for a in ("z", "y", "x", "c"))
    tp = x * 2 + c
    NP, NM = Z // 2, (Z - 1) // 2
    up = (lax.rem(z + 1, Z), y, x, c)
    down = (lax.rem(z + Z - 1, Z), y, x, c)
    sib = (z, y, x, 1 - c)

    def ymod(k):
        return lax.rem(y + k, Y)

    def xmod(k):
        return lax.rem(x + k, X)

    def zmod(k):
        return lax.rem(z + k + Z, Z)

    phase("barrier")
    barrier = pltpu.get_barrier_semaphore()
    peers = [up, down] + [(z, ymod(k), x, c) for k in range(1, Y)]
    peers += [(z, y, lax.rem(tp + k, TPN) // 2, lax.rem(lax.rem(tp + k, TPN), 2)) for k in range(1, TPN)]
    for peer in peers:
        pl.semaphore_signal(barrier, inc=1, device_id=peer, device_id_type=MESH)

    loads = [(tok_hbm, tok), (ing_hbm, ing), (wb_hbm, b16), (dr_hbm, dr), (og_hbm, gain_ref)]
    loads += [(ref, w_ref.at[:, i * DK : (i + 1) * DK]) for i, ref in enumerate((wq_hbm, wk_hbm, wv_hbm, wg_hbm, wo_hbm))]
    loads += [(ref, taps_b.at[i]) for i, ref in enumerate((cq_hbm, ck_hbm, cv_hbm))]
    loads = [pltpu.make_async_copy(src, dst, in_s.at[i]) for i, (src, dst) in enumerate(loads)]
    for cp in loads:
        cp.start()
    for cp in loads:
        cp.wait()
    t = tok[...].astype(f32)
    t = t * lax.rsqrt(jnp.mean(t * t, axis=-1, keepdims=True) + epsilon)
    tokf[...] = t * ing[...].reshape(1, 1, D)
    for s in range(Y):
        x_ref[s, 0:NB, :] = tokf[:, s, :].astype(bf16)
    part = lax.rem(z * Y + y, 8)
    lane = lax.broadcasted_iota(jnp.int32, (1, DK), 1)
    b = jnp.concatenate([b16[...].astype(f32)] * 8, axis=1)
    b_ref[...] = jnp.where(lane // ROWS == part, b, 0.0)
    pl.semaphore_wait(barrier, len(peers))

    phase("send_own")
    copies = []

    def go(cp):
        cp.start()
        copies.append(cp)

    def rows_of(zz, yy):
        return pl.ds(pl.multiple_of((zz * Y + yy) * ROWS, ROWS), ROWS)

    own = rows_of(z, y)
    local = pltpu.make_async_copy(w_ref, wbuf.at[own], l_s.at[0])
    local.start()
    local_b = pltpu.make_async_copy(b_ref, bbuf.at[z, y], l_s.at[1])
    local_b.start()
    for k in range(1, Y):
        go(copy_to(w_ref, wbuf.at[own], wy_s.at[k], wy_r.at[k], (z, ymod(k), x, c)))
        go(copy_to(b_ref, bbuf.at[z, y], by_s.at[k], by_r.at[k], (z, ymod(k), x, c)))
    go(copy_to(w_ref, wbuf.at[own], wz_s.at[0, 1, 0], wz_r.at[0, 1, 0], up))
    if NM:
        go(copy_to(w_ref, wbuf.at[own], wz_s.at[1, 1, 0], wz_r.at[1, 1, 0], down))
    slot0 = tp * Y
    for k in range(1, Y):
        go(copy_to(x_ref.at[ymod(k)], xbuf.at[slot0 + y], xy_s.at[k], xy_r.at[k], (z, ymod(k), x, c)))
    local_x = pltpu.make_async_copy(x_ref.at[y], xbuf.at[slot0 + y], l_s.at[2])
    local_x.start()
    HALO = TPN * Y
    last_tp = jnp.logical_and(x == X - 1, c == 1)
    tail_owner = jnp.logical_and(last_tp, y == Y - 1)

    @pl.when(tail_owner)
    def _():
        copy_to(x_ref, hin, hz_s, hz_r, up).start()

    phase("w_y")
    for k in range(1, Y):
        blk = rows_of(z, ymod(Y - k))
        copy_to(w_ref, wbuf.at[blk], wy_s.at[k], wy_r.at[k], sib).wait_recv()
    for d in range(1, Y):
        blk = rows_of(z, ymod(d))
        go(copy_to(wbuf.at[blk], wbuf.at[blk], wz_s.at[0, 1, d], wz_r.at[0, 1, d], up))
        if NM:
            go(copy_to(wbuf.at[blk], wbuf.at[blk], wz_s.at[1, 1, d], wz_r.at[1, 1, d], down))
    for k in range(1, Y):
        copy_to(b_ref, bbuf.at[z, ymod(Y - k)], by_s.at[k], by_r.at[k], sib).wait_recv()
    local_b.wait()
    go(copy_to(bbuf.at[z], bbuf.at[z], bz_s.at[0, 1], bz_r.at[0, 1], up))
    if NM:
        go(copy_to(bbuf.at[z], bbuf.at[z], bz_s.at[1, 1], bz_r.at[1, 1], down))

    phase("tok_y")
    for k in range(1, Y):
        copy_to(x_ref.at[0], xbuf.at[slot0 + ymod(Y - k)], xy_s.at[k], xy_r.at[k], sib).wait_recv()
    local_x.wait()
    mine = pl.ds(slot0, Y)
    for k in range(1, X):
        go(copy_to(xbuf.at[mine], xbuf.at[mine], xx_s.at[k], xx_r.at[k], (z, y, xmod(k), c)))
    go(copy_to(xbuf.at[mine], xbuf.at[mine], xc_s.at[0], xc_r.at[0], sib))

    def w_step(k, plus, fplus, minus, fminus):
        for d in range(Y):
            if plus:
                blk = rows_of(zmod(-k), ymod(d))
                copy_to(wbuf.at[blk], wbuf.at[blk], wz_s.at[0, k, d], wz_r.at[0, k, d], up).wait_recv()
                if fplus:
                    copy_to(wbuf.at[blk], wbuf.at[blk], wz_s.at[0, k + 1, d], wz_r.at[0, k + 1, d], up).start()
            if minus:
                blk = rows_of(zmod(k), ymod(d))
                copy_to(wbuf.at[blk], wbuf.at[blk], wz_s.at[1, k, d], wz_r.at[1, k, d], down).wait_recv()
                if fminus:
                    copy_to(wbuf.at[blk], wbuf.at[blk], wz_s.at[1, k + 1, d], wz_r.at[1, k + 1, d], down).start()
        if plus:
            g = bbuf.at[zmod(-k)]
            copy_to(g, g, bz_s.at[0, k], bz_r.at[0, k], up).wait_recv()
            if fplus:
                copy_to(g, g, bz_s.at[0, k + 1], bz_r.at[0, k + 1], up).start()
        if minus:
            g = bbuf.at[zmod(k)]
            copy_to(g, g, bz_s.at[1, k], bz_r.at[1, k], down).wait_recv()
            if fminus:
                copy_to(g, g, bz_s.at[1, k + 1], bz_r.at[1, k + 1], down).start()

    def ring(step, pauses={}):
        for k in range(1, NP + 1):
            step(k, True, k < NP, k <= NM, k < NM)
            if k in pauses:
                pauses[k]()

    def halo_forwards():
        @pl.when(tail_owner)
        def _():
            copy_to(x_ref, hin, hz_s, hz_r, up).wait_recv()
            for k in range(1, Y):
                copy_to(hin.at[ymod(k)], xbuf.at[HALO], hy_s.at[k], hy_r, (z, ymod(k), x, c)).start()
            cp = pltpu.make_async_copy(hin.at[y], xbuf.at[HALO], l_s.at[3])
            cp.start()
            cp.wait()

        @pl.when(jnp.logical_and(last_tp, y != Y - 1))
        def _():
            copy_to(hin.at[0], xbuf.at[HALO], hy_s.at[0], hy_r, sib).wait_recv()

        @pl.when(last_tp)
        def _():
            for k in range(1, X):
                copy_to(xbuf.at[HALO], xbuf.at[HALO], hx_s.at[k], hx_r, (z, y, xmod(k), c)).start()

    def token_forwards():
        for k in range(1, X):
            got = pl.ds((xmod(X - k) * 2 + c) * Y, Y)
            copy_to(xbuf.at[got], xbuf.at[got], xx_s.at[k], xx_r.at[k], sib).wait_recv()
            go(copy_to(xbuf.at[got], xbuf.at[got], xc_s.at[k], xc_r.at[k], sib))

        @pl.when(c == 1)
        def _():
            @pl.when(x != X - 1)
            def _():
                copy_to(xbuf.at[HALO], xbuf.at[HALO], hx_s.at[0], hx_r, sib).wait_recv()

            copy_to(xbuf.at[HALO], xbuf.at[HALO], hc_s, hc_r, sib).start()

    phase("w_ring")
    ring(w_step, {1: halo_forwards, min(3, NP): token_forwards})

    phase("tok_sib")
    sc = (1 - c)
    for k in range(X):
        got = pl.ds((xmod(X - k) * 2 + sc) * Y, Y)
        copy_to(xbuf.at[got], xbuf.at[got], xc_s.at[k], xc_r.at[k], sib).wait_recv()

    @pl.when(c == 0)
    def _():
        copy_to(xbuf.at[HALO], xbuf.at[HALO], hc_s, hc_r, sib).wait_recv()

    local.wait()

    phase("proj")
    PR = TPN * Y * PB
    xs = xbuf[...].reshape(PR + PB, D)
    pre = jnp.dot(xs, wbuf[:, : 4 * DK], preferred_element_type=f32).astype(bf16).astype(f32)
    bsum = jnp.sum(bbuf[...].reshape(D // DK, 8, DK), axis=1)
    for j in range(D // DK):
        wbt[:, j * DK : (j + 1) * DK] = jnp.broadcast_to(bsum[j : j + 1, :], (DK, DK)).astype(bf16)
    bpre = dot_nt(xs, wbt[...]).astype(bf16).astype(f32)
    started = jnp.where(z > 0, 1.0, 0.0).astype(f32)
    ext[8 - (TAPS - 1) : 8, :] = pre[PR + NB - (TAPS - 1) : PR + NB, :] * started
    for yy in range(Y):
        for t in range(TPN):
            row = (t * Y + yy) * PB
            to = (yy * TPN + t) * NB
            ext[8 + to : 8 + to + NB, :] = pre[row : row + NB, :]
            bext[to : to + NB, :] = bpre[row : row + NB, :]

    phase("wo_t")
    for j in range(D // DK):
        tile = wbuf[j * DK : (j + 1) * DK, 4 * DK : 5 * DK].astype(f32)
        wo[tp, :, j * DK : (j + 1) * DK] = tile.T.astype(bf16)

    phase("conv")
    taps = [taps_b[i].astype(f32) for i in range(3)]
    outs = []
    for kind in range(3):
        lanes = slice(kind * DK, (kind + 1) * DK)
        acc = jnp.zeros((NT, DK), f32)
        for j in range(TAPS):
            at = 8 - (TAPS - 1) + j
            acc = acc + ext[at : at + NT, lanes] * taps[kind][j : j + 1, :]
        outs.append(acc * jax.nn.sigmoid(acc))
    q, k_, v = outs
    qs[...] = q * (lax.rsqrt(jnp.sum(q * q, axis=1, keepdims=True) + epsilon) * DK ** (-0.5))
    ks[...] = k_ * lax.rsqrt(jnp.sum(k_ * k_, axis=1, keepdims=True) + epsilon)
    vs[...] = v
    total_tokens = NT * Z
    bs[...] = jax.nn.sigmoid(bext[...] + math.log(DK / (4.0 * total_tokens)))

    for k in range(1, X):
        go(copy_to(wo.at[tp], wo.at[tp], ox_s.at[k], ox_r.at[k], (z, y, xmod(k), c)))
    go(copy_to(wo.at[tp], wo.at[tp], oc_s.at[0], oc_r.at[0], sib))

    phase("chunks")
    rate = jnp.broadcast_to(dr[...], (1, DK)) * (1.0 / (NT * Z))
    ri = lax.broadcasted_iota(jnp.int32, (CH, CH), 0)
    ci = lax.broadcasted_iota(jnp.int32, (CH, CH), 1)
    rl = lax.broadcasted_iota(jnp.int32, (CH, DK), 0).astype(f32)
    rate_c = rate[:, :CH]
    decay = jnp.where(ri >= ci, jnp.exp(-rate_c * (ri - ci).astype(f32)), 0.0)
    down_row = jnp.exp(-rate * (rl + 1.0))
    up_row = jnp.exp(-rate * (CH - 1.0 - rl))
    kept = jnp.exp(-rate * CH)
    eye = jnp.where(
        lax.broadcasted_iota(jnp.int32, (DK, DK), 0) == lax.broadcasted_iota(jnp.int32, (DK, DK), 1), 1.0, 0.0
    ).astype(f32)
    prefix = None
    for i in range(NT // CH):
        rows = slice(i * CH, (i + 1) * CH)
        q, k_, v, b = qs[rows, :], ks[rows, :], vs[rows, :], bs[rows, :]
        kb = k_ * b
        lower = jnp.where(ri > ci, dot_nt(kb, k_) * decay, 0.0)
        scores = dot_nt(q, k_) * decay
        near = jnp.where(ri // INNER == ci // INNER, lower, 0.0)
        inverse = jnp.where(ri == ci, 1.0, 0.0) - near
        power = dot(near, near)
        span = 2
        while span < INNER:
            inverse = inverse + dot(inverse, power)
            span *= 2
            if span < INNER:
                power = dot(power, power)
        span = INNER
        while span < CH:
            part = jnp.where(
                jnp.logical_and(ri // (2 * span) == ci // (2 * span), ri // span != ci // span), lower, 0.0
            )
            inverse = inverse - dot(inverse, dot(part, inverse))
            span *= 2
        both = dot(inverse, jnp.concatenate([kb * down_row, v * b], axis=1))
        inner = dot(scores, both)
        reach = q * down_row - inner[:, :DK]
        kd = (k_ * up_row).T
        tail = dot(kd, both)
        step_map = kept * eye - tail[:, :DK]
        if prefix is None:
            rdo[rows, :] = reach
            olo[rows, :] = inner[:, DK:]
            prefix = jnp.concatenate([step_map, tail[:, DK:]], axis=1)
        else:
            seen = dot(reach, prefix)
            rdo[rows, :] = seen[:, :DK]
            olo[rows, :] = inner[:, DK:] + seen[:, DK:]
            prefix = dot(step_map, prefix)
            prefix = jnp.concatenate([prefix[:, :DK], prefix[:, DK:] + tail[:, DK:]], axis=1)
    kappa = jnp.exp(-rate * NT)
    mbuf[z, :, :DK] = (prefix[:, :DK] - kappa * eye).astype(bf16)
    mbuf[z, :, DK:] = prefix[:, DK:].astype(bf16)

    phase("map_send")
    NCH = mz_s.shape[2]
    PIECE = DK // NCH

    def piece(zz, d):
        return mbuf.at[zz, pl.ds(d * PIECE, PIECE)]

    for d in range(NCH):
        go(copy_to(piece(z, d), piece(z, d), mz_s.at[0, 1, d], mz_r.at[0, 1, d], up))
        if NM:
            go(copy_to(piece(z, d), piece(z, d), mz_s.at[1, 1, d], mz_r.at[1, 1, d], down))

    near_d, near_u, far = ext.at[0:DK, 0:DK], ext.at[0:DK, DK : 2 * DK], ext.at[0:DK, 2 * DK : 3 * DK]

    near_d[...] = jnp.zeros((DK, DK), f32)
    near_u[...] = jnp.zeros((DK, DK), f32)
    far[...] = jnp.zeros((DK, DK), f32)

    def m_step(k, plus, fplus, minus, fminus):
        for d in range(NCH):
            if plus:
                p = piece(zmod(-k), d)
                copy_to(p, p, mz_s.at[0, k, d], mz_r.at[0, k, d], up).wait_recv()
                if fplus:
                    copy_to(p, p, mz_s.at[0, k + 1, d], mz_r.at[0, k + 1, d], up).start()
            if minus:
                p = piece(zmod(k), d)
                copy_to(p, p, mz_s.at[1, k, d], mz_r.at[1, k, d], down).wait_recv()
                if fminus:
                    copy_to(p, p, mz_s.at[1, k + 1, d], mz_r.at[1, k + 1, d], down).start()
        if plus:
            got = mbuf[zmod(-k)]
            kk = k * 1.0 if isinstance(k, int) else k.astype(f32)
            scale = jnp.exp(-rate * NT * (kk - 1.0))
            valid = jnp.where(z >= k, 1.0, 0.0).astype(f32)
            nd, nu = near_d[...], near_u[...]
            prod = dot(nd, got)
            gd, gu = got[:, :DK].astype(f32), got[:, DK:].astype(f32)
            near_d[...] = kappa * nd + scale * gd + prod[:, :DK]
            near_u[...] = nu + valid * (scale * gu + prod[:, DK:])
        if minus:
            got = mbuf[zmod(k)]
            valid = jnp.where(z + k >= Z, 1.0, 0.0).astype(f32)
            s = far[...]
            far[...] = kappa * s + dot(got[:, :DK], s) + valid * got[:, DK:].astype(f32)

    phase("map_ring")
    ring(m_step)

    phase("wo_fwd")
    for k in range(1, X):
        h = xmod(X - k) * 2 + c
        copy_to(wo.at[h], wo.at[h], ox_s.at[k], ox_r.at[k], sib).wait_recv()
        go(copy_to(wo.at[h], wo.at[h], oc_s.at[k], oc_r.at[k], sib))

    phase("final")
    s = far[...]
    state = jnp.exp(-rate * NT * NP) * s + dot(near_d[...], s) + near_u[...]
    o = olo[...] + dot(rdo[...], state)
    gate = ext[8 : 8 + NT, 3 * DK : 4 * DK]
    o = o * lax.rsqrt(jnp.mean(o * o, axis=1, keepdims=True) + out_epsilon) * gain_ref[...]
    olo[...] = o * (gate * jax.nn.sigmoid(gate))
    for yy in range(Y):
        for t in range(TPN):
            to = (yy * TPN + t) * NB
            gsend[t, yy, 0:NB, :] = olo[to : to + NB, :].astype(bf16)
    phase("g_send")
    for k in range(1, TPN):
        t = lax.rem(tp + k, TPN)
        go(copy_to(gsend.at[t], grecv.at[tp], g_s.at[k], g_r.at[k], (z, y, t // 2, lax.rem(t, 2))))
    grecv[tp] = gsend[tp]
    for k in range(X):
        h = xmod(X - k) * 2 + sc
        copy_to(wo.at[h], wo.at[h], oc_s.at[k], oc_r.at[k], sib).wait_recv()
    for k in range(1, TPN):
        t = lax.rem(tp + TPN - k, TPN)
        copy_to(gsend.at[0], grecv.at[t], g_s.at[k], g_r.at[k], sib).wait_recv()
    phase("out_mm")
    gated = jnp.concatenate([grecv[t].reshape(Y * PB, DK) for t in range(TPN)], axis=1)
    res = jnp.dot(gated, wo[...].reshape(TPN * DK, D), preferred_element_type=f32)

    def put(row, block):
        for s in range(Y):
            @pl.when(row == s)
            def _():
                tokf[:, s, :] = block[0:NB, :].astype(f32)

    obuf[0] = res.astype(bf16).reshape(Y, PB, D)
    for k in range(1, Y):
        go(copy_to(obuf.at[0, ymod(k)], obuf.at[1, y], o_s.at[k], o_r.at[k], (z, ymod(k), x, c)))
    put(y, obuf[0, y])
    phase("o_recv")
    for k in range(1, Y):
        src = ymod(Y - k)
        copy_to(obuf.at[0, 0], obuf.at[1, src], o_s.at[k], o_r.at[k], sib).wait_recv()
        put(src, obuf[1, src])
    out_ref[...] = tokf[...].astype(bf16)

    phase("drain")
    for cp in copies:
        cp.wait_send()
    for d, steps in ((0, NP), (1, NM)):
        for k in range(2, steps + 1):
            to = up if d == 0 else down
            for e in range(Y):
                copy_to(w_ref, wbuf.at[own], wz_s.at[d, k, e], wz_r.at[d, k, e], to).wait_send()
            copy_to(bbuf.at[0], bbuf.at[0], bz_s.at[d, k], bz_r.at[d, k], to).wait_send()
            for e in range(NCH):
                copy_to(piece(z, e), piece(z, e), mz_s.at[d, k, e], mz_r.at[d, k, e], to).wait_send()

    @pl.when(tail_owner)
    def _():
        copy_to(x_ref, hin, hz_s, hz_r, up).wait_send()
        for k in range(1, Y):
            copy_to(hin.at[0], xbuf.at[HALO], hy_s.at[k], hy_r, sib).wait_send()

    @pl.when(last_tp)
    def _():
        for k in range(1, X):
            copy_to(xbuf.at[HALO], xbuf.at[HALO], hx_s.at[k], hx_r, sib).wait_send()

    @pl.when(c == 1)
    def _():
        copy_to(xbuf.at[HALO], xbuf.at[HALO], hc_s, hc_r, sib).wait_send()
    phase(None)


def shards(
    sizes, tokens, in_gain, w_query, w_key, w_value, w_gate, w_beta,
    conv_query, conv_key, conv_value, decay_rate, out_gain, w_out,
):
    Z, Y, X = sizes
    NB, seqs, D = tokens.shape
    PB = -(-NB // 16) * 16
    TPN = 2 * X
    NT = Y * TPN * NB
    CH = 128 if NT % 128 == 0 else 96
    NCH = 4
    D1 = pltpu.SemaphoreType.DMA
    NP = Z // 2
    scratch = [
        pltpu.VMEM((NB, seqs, D), bf16),
        pltpu.VMEM((NB, seqs, D), f32),
        pltpu.VMEM((1, D), f32),
        pltpu.VMEM((seqs, PB, D), bf16),
        pltpu.VMEM((ROWS, 5 * DK), bf16),
        pltpu.VMEM((1, ROWS), bf16),
        pltpu.VMEM((1, DK), f32),
        pltpu.VMEM((3, TAPS, DK), bf16),
        pltpu.VMEM((1, 1), f32),
        pltpu.VMEM((1, DK), f32),
        D1((13,)),
        pltpu.VMEM((D, 5 * DK), bf16),
        pltpu.VMEM((Z, Y, 1, DK), f32),
        pltpu.VMEM((DK, D), bf16),
        pltpu.VMEM((TPN * Y + 1, PB, D), bf16),
        pltpu.VMEM((Y, PB, D), bf16),
        pltpu.VMEM((8 + max(NT, DK), 4 * DK), f32),
        pltpu.VMEM((NT, DK), f32),
        pltpu.VMEM((NT, DK), f32),
        pltpu.VMEM((NT, DK), f32),
        pltpu.VMEM((NT, DK), f32),
        pltpu.VMEM((NT, DK), f32),
        pltpu.VMEM((NT, DK), f32),
        pltpu.VMEM((NT, DK), f32),
        pltpu.VMEM((Z, DK, 2 * DK), bf16),
        pltpu.VMEM((TPN, DK, D), bf16),
        pltpu.VMEM((TPN, Y, PB, DK), bf16),
        pltpu.VMEM((TPN, Y, PB, DK), bf16),
        pltpu.VMEM((2, Y, PB, D), bf16),
    ]
    sems = [
        D1((Y,)), D1((Y,)), D1((Y,)), D1((Y,)),
        D1((2, NP + 1, Y)), D1((2, NP + 1, Y)), D1((2, NP + 1)), D1((2, NP + 1)),
        D1((Y,)), D1((Y,)), D1(()), D1(()), D1((Y,)), D1(()), D1((X,)), D1(()),
        D1(()), D1(()), D1((X,)), D1((X,)), D1((X,)), D1((X,)),
        D1((X,)), D1((X,)), D1((X,)), D1((X,)),
        D1((2, NP + 1, NCH)), D1((2, NP + 1, NCH)), D1((TPN,)), D1((TPN,)), D1((Y,)), D1((Y,)), D1((4,)),
    ]
    out = pl.pallas_call(
        functools.partial(mixer, (Z, Y, X, NB, PB, CH)),
        out_shape=jax.ShapeDtypeStruct((NB, seqs, D), bf16),
        in_specs=[pl.BlockSpec(memory_space=pltpu.HBM)] * 13,
        out_specs=pl.BlockSpec(memory_space=pltpu.VMEM),
        scratch_shapes=scratch + sems,
        compiler_params=pltpu.CompilerParams(collective_id=0, has_side_effects=True),
        name="mixer",
    )(
        tokens, in_gain.reshape(1, D), w_query, w_key, w_value, w_gate, w_out.T, w_beta.T,
        conv_query, conv_key, conv_value, decay_rate.reshape(1, 1), out_gain.reshape(1, DK),
    )
    return out


def solution(mesh, sizes=(16, 4, 4)):
    Z, Y, X = sizes
    finer = Mesh(mesh.devices.reshape(Z, Y, X, 2), ("z", "y", "x", "c"))
    return jax.shard_map(
        functools.partial(shards, sizes),
        mesh=finer,
        in_specs=(
            P(SP + TP, None, None), P(), P(SP, TP), P(SP, TP), P(SP, TP), P(SP, TP), P(SP, TP),
            P(None, TP), P(None, TP), P(None, TP), P(TP), P(), P(TP, SP),
        ),
        out_specs=P(SP + TP, None, None),
        check_vma=False,
    )
```
